32 devices in a mesh: sp: 16 (over z, y, core), tp: 2 (over x).
Axes of the slice: x: 2, y: 2, z: 4, core: 2. Of those that a mesh axis runs over, the one named last changes fastest.
Arguments:
- residual: bfloat16 [2048, 2048], P(('sp', 'tp')), may hold values from -6 to 6
- forget_forward: bfloat16 [2048, 1024], P('sp', 'tp'), may hold values from -5.5 to 5.5
- forget_backward: bfloat16 [2048, 1024], P('sp', 'tp'), may hold values from -5.5 to 5.5
- value_written: bfloat16 [2048, 1024], P('sp', 'tp'), may hold values from -6 to 6
- query_logits: bfloat16 [2048, 1024], P('sp', 'tp'), may hold values from -6 to 6
- output_gate_logits: bfloat16 [2048, 1024], P('sp', 'tp'), may hold values from -6 to 6
- forget_minimum: float32 [2, 1024], P(None, 'tp'), may hold values from 0.88 to 1
- extra_log_rate: float32 [2, 2048, 8], P(None, 'sp', 'tp'), may hold values from -0.7 to 0
- head_norm_scale: float32 [128], replicated, may hold values from 0.1 to 1.9
- output_matrix: bfloat16 [1024, 2048], P(None, 'sp'), may hold values from -0.1875 to 0.1875
- prenorm_scale: float32 [2048], replicated, may hold values from 0.1 to 1.9
- gate_up_matrix: bfloat16 [2048, 5632], P('sp', 'tp'), may hold values from -0.125 to 0.125
- value_up_matrix: bfloat16 [2048, 5632], P('sp', 'tp'), may hold values from -0.125 to 0.125
- gate_taps: float32 [3, 5632], P(None, 'tp'), may hold values from -3.5 to 3.5
- value_taps: float32 [3, 5632], P(None, 'tp'), may hold values from -3.5 to 3.5
- down_matrix: bfloat16 [5632, 2048], P('tp', 'sp'), may hold values from -0.078125 to 0.078125
Outputs:
- layer_out: bfloat16 [2048, 2048], P(('sp', 'tp'))
The draws below stay inside these ranges and needn't reach their ends.
All inputs are finite; a program needn't handle non-finite values.
Results may differ from the reference program's by a relative error of at most 0.012.
Values may be sent and summed in bfloat16 or wider, within the bound.
A program may use at most 128 MiB of HBM per device.

```python
import jax
import jax.numpy as jnp
from jax import lax

D = 2048
HEADS = 8
HEAD_WIDTH = 128
HW = 1024
FF = 5632
BLOCK = 64
TOK_DEV = 128
TOKENS = 2048
N_TP = 2


def forget_draw(key):
    noise = jnp.clip(jax.random.normal(jax.random.fold_in(key, 1), (TOKENS, HEADS * HEAD_WIDTH), jnp.float32), -4.0, 4.0)
    shifts = jax.random.uniform(jax.random.fold_in(key, 2), (TOKENS // TOK_DEV, 1, 1), jnp.float32, -1.5, 1.5)
    noise = (noise.reshape(TOKENS // TOK_DEV, TOK_DEV, HEADS * HEAD_WIDTH) + shifts).reshape(TOKENS, HEADS * HEAD_WIDTH)
    return noise.astype(jnp.bfloat16)


def draw_forget_forward(key, part):
    return forget_draw(jax.random.fold_in(key, 11))


def draw_forget_backward(key, part):
    return forget_draw(jax.random.fold_in(key, 12))


def draw_forget_minimum(key, part):
    fast_count = 4
    picks = jax.random.randint(jax.random.fold_in(key, 21), (2, HEADS, 1), 0, 8)
    fast_bound = jax.random.uniform(jax.random.fold_in(key, 22), (2, HEADS, HEAD_WIDTH), jnp.float32, 0.88, 0.92)
    slow_bound = 1.0 - jax.random.uniform(jax.random.fold_in(key, 23), (2, HEADS, HEAD_WIDTH), jnp.float32, 0.5, 1.5) / TOKENS
    forget_floor = jnp.where(picks < fast_count, fast_bound, slow_bound)
    return forget_floor.reshape(2, HEADS * HEAD_WIDTH).astype(jnp.float32)


def draw_extra_log_rate(key, part):
    spots = jax.random.randint(jax.random.fold_in(key, 31), (2, 1, 3), 0, TOKENS)
    places = jnp.arange(TOKENS, dtype=jnp.int32)[None, :, None]
    struck = jnp.any(places == spots, axis=-1)[:, :, None]
    depth = jnp.log(jax.random.uniform(jax.random.fold_in(key, 32), (2, TOKENS, HEADS), jnp.float32, 0.5, 0.8))
    return jnp.where(struck, depth, 0.0).astype(jnp.float32)


def block_levels(own_key, shape, cuts, least, top_value):
    gain = 1.0
    for dim, parts in cuts:
        heights = jax.random.uniform(jax.random.fold_in(jax.random.fold_in(own_key, 6), dim), (parts,), jnp.float32, least / len(cuts), top_value / len(cuts))
        gain = gain * jnp.repeat(jnp.exp(heights), shape[dim] // parts).reshape((-1,) + (1,) * (len(shape) - 1 - dim))
    return gain


def normal_values(rng, extent, scale, bound, cuts=(), kind=jnp.bfloat16):
    result = scale * jax.random.normal(rng, extent, jnp.float32)
    if cuts:
        result = result * block_levels(rng, extent, cuts, -0.22, 0.18)
    return jnp.clip(result, -bound, bound).astype(kind)


def setup_inputs(seed: int = 0) -> dict:
    seeds = jax.random.split(jax.random.key(seed), 17)
    residual = normal_values(seeds[0], (TOKENS, D), 1.0, 6.0, ((0, 32),))
    forget_forward = draw_forget_forward(jax.random.fold_in(seeds[16], 71), 0)
    forget_backward = draw_forget_backward(jax.random.fold_in(seeds[16], 71), 0)
    value_written = normal_values(seeds[3], (TOKENS, HW), 1.0, 6.0, ((0, 16), (1, 2)))
    query_logits = normal_values(seeds[4], (TOKENS, HW), 1.0, 6.0, ((0, 16), (1, 2)))
    output_gate_logits = normal_values(seeds[5], (TOKENS, HW), 1.0, 6.0, ((0, 16), (1, 2)))
    forget_minimum = draw_forget_minimum(jax.random.fold_in(seeds[16], 71), 0)
    extra_log_rate = draw_extra_log_rate(jax.random.fold_in(seeds[16], 71), 0)
    head_norm_scale = jnp.clip(1.0 + 0.18 * jax.random.normal(seeds[8], (HEAD_WIDTH,), jnp.float32), 0.1, 1.9)
    output_matrix = normal_values(seeds[9], (HW, D), HW ** -0.5, 0.1875, ((1, 16),))
    prenorm_scale = jnp.clip(1.0 + 0.18 * jax.random.normal(seeds[10], (D,), jnp.float32), 0.1, 1.9)
    gate_up_matrix = normal_values(seeds[11], (D, FF), D ** -0.5, 0.125, ((0, 16), (1, 2)))
    value_up_matrix = normal_values(seeds[12], (D, FF), D ** -0.5, 0.125, ((0, 16), (1, 2)))
    gate_taps = normal_values(seeds[13], (3, FF), 3 ** -0.5, 3.5, ((1, 2),), jnp.float32)
    value_taps = normal_values(seeds[14], (3, FF), 3 ** -0.5, 3.5, ((1, 2),), jnp.float32)
    down_matrix = normal_values(seeds[15], (FF, D), FF ** -0.5, 0.078125, ((0, 2), (1, 16)))
    return dict(residual=residual, forget_forward=forget_forward, forget_backward=forget_backward, value_written=value_written, query_logits=query_logits, output_gate_logits=output_gate_logits, forget_minimum=forget_minimum, extra_log_rate=extra_log_rate, head_norm_scale=head_norm_scale, output_matrix=output_matrix, prenorm_scale=prenorm_scale, gate_up_matrix=gate_up_matrix, value_up_matrix=value_up_matrix, gate_taps=gate_taps, value_taps=value_taps, down_matrix=down_matrix)


EPSILON = 1e-06

def rms_scale(array):
    return array * lax.rsqrt(lax.optimization_barrier(jnp.mean(array * array, axis=-1, keepdims=True)) + EPSILON)

def forget_factors(forget_logits, forget_floor, extra_decay):
    unbounded_gate = forget_logits.astype(jnp.float32)
    log_forget_gate = jnp.log(forget_floor + (1.0 - forget_floor) * jax.nn.sigmoid(unbounded_gate)) + jnp.repeat(extra_decay, HEAD_WIDTH, axis=1)
    key_in = (1.0 - forget_floor) * jax.nn.sigmoid(-unbounded_gate)
    shape = (unbounded_gate.shape[0], unbounded_gate.shape[1] // HEAD_WIDTH, HEAD_WIDTH)
    return (log_forget_gate.reshape(shape), key_in.reshape(shape))

def block_scan(log_forget_gate, key_in, values, queries):
    length, heads, depth = log_forget_gate.shape
    width = values.shape[2]
    blocks = length // BLOCK
    highest = lax.Precision.HIGHEST
    lower = jnp.tril(jnp.ones((BLOCK, BLOCK), dtype=bool))[:, :, None, None]

    def split(array):
        return array.reshape(blocks, BLOCK, heads, array.shape[2])

    def advance(carry, pieces):
        state, carried = carry
        log_part, key_part, value_part, query_part = pieces
        running = jnp.cumsum(log_part, axis=0)
        block_total = running[-1]
        query_carry = query_part * jnp.exp(carried[None] + running)
        from_state = jnp.einsum('chd,hde->che', query_part * jnp.exp(running), state, precision=highest)
        gaps = jnp.where(lower, running[:, None] - running[None, :], -1e+30)
        scores = jnp.einsum('ihd,jhd,ijhd->hij', query_part, key_part, jnp.exp(gaps), precision=highest)
        inside = jnp.einsum('hij,jhe->ihe', scores, value_part, precision=highest)
        fresh = jnp.einsum('chd,che->hde', key_part * jnp.exp(block_total[None] - running), value_part, precision=highest)
        state = jnp.exp(block_total)[:, :, None] * state + fresh
        return ((state, carried + block_total), (from_state + inside, query_carry))
    start = (jnp.zeros((heads, depth, width), jnp.float32), jnp.zeros((heads, depth), jnp.float32))
    (state, carried), (outputs, query_carry) = lax.scan(advance, start, (split(log_forget_gate), split(key_in), split(values), split(queries)))
    return (state, carried, outputs.reshape(length, heads, width), query_carry.reshape(length, heads, depth))

def reference(residual, forget_forward, forget_backward, value_written, query_logits, output_gate_logits, forget_minimum, extra_log_rate, head_norm_scale, output_matrix, prenorm_scale, gate_up_matrix, value_up_matrix, gate_taps, value_taps, down_matrix):
    length = value_written.shape[0]
    shape = (length, value_written.shape[1] // HEAD_WIDTH, HEAD_WIDTH)
    values = value_written.astype(jnp.float32).reshape(shape)
    queries = jax.nn.silu(query_logits.astype(jnp.float32)).reshape(shape)
    log_decay_forward, key_forward = forget_factors(forget_forward, forget_minimum[0], extra_log_rate[0])
    forward = block_scan(log_decay_forward, key_forward, values, queries)[2]
    log_decay_backward, key_backward = forget_factors(forget_backward, forget_minimum[1], extra_log_rate[1])
    backward = block_scan(log_decay_backward[::-1], key_backward[::-1], values[::-1], queries[::-1])[2][::-1]
    gated = rms_scale(forward + backward) * head_norm_scale * jax.nn.silu(output_gate_logits.astype(jnp.float32)).reshape(shape)
    mixed_in = gated.reshape(length, shape[1] * HEAD_WIDTH).astype(jnp.bfloat16)
    after_mix = residual.astype(jnp.float32) + jnp.dot(mixed_in, output_matrix, preferred_element_type=jnp.float32)
    normed = (rms_scale(after_mix) * prenorm_scale).astype(jnp.bfloat16)
    gate_up = jnp.dot(normed, gate_up_matrix, preferred_element_type=jnp.float32).astype(jnp.bfloat16)
    value_up = jnp.dot(normed, value_up_matrix, preferred_element_type=jnp.float32).astype(jnp.bfloat16)

    def convolve(upward, kernel):
        padded = jnp.pad(upward, ((1, 1), (0, 0)))
        return padded[:length] * kernel[0] + padded[1:length + 1] * kernel[1] + padded[2:] * kernel[2]
    hidden = (jax.nn.silu(convolve(gate_up, gate_taps)) * convolve(value_up, value_taps)).astype(jnp.bfloat16)
    group_width = hidden.shape[1] // N_TP

    def add_group(index, total):
        first = (index * group_width).astype(jnp.int32)
        hidden_part = lax.dynamic_slice_in_dim(hidden, first, group_width, 1)
        weight_part = lax.dynamic_slice_in_dim(down_matrix, first, group_width, 0)
        partial_sum = jnp.dot(hidden_part, weight_part, preferred_element_type=jnp.float32)
        return total + lax.optimization_barrier(partial_sum.astype(jnp.bfloat16)).astype(jnp.float32)
    down = lax.fori_loop(jnp.int32(0), jnp.int32(N_TP), add_group, jnp.zeros((length, down_matrix.shape[1]), jnp.float32))
    return (after_mix + down).astype(jnp.bfloat16)
```

```python
import functools
import math

import jax
import jax.numpy as jnp
from jax import lax
from jax.experimental import pallas as pl
from jax.experimental.pallas import tpu as pltpu
from jax.sharding import PartitionSpec as P

HEAD_WIDTH = 128
EPSILON = 1e-06
MESH = pl.DeviceIdType.MESH
F32 = jnp.float32
BF16 = jnp.bfloat16
DECAY_ROWS = 16


class Grid:
    def __init__(self, mesh):
        sp, tp = mesh.shape["sp"], mesh.shape["tp"]
        self.sp, self.x = sp, tp
        self.c = math.gcd(sp, 2)
        self.y = math.gcd(sp // self.c, 2)
        self.z = sp // (self.c * self.y)
        self.ids = iter(range(100))

    def size(self, dim):
        return getattr(self, dim)

    def place(self):
        s, t = lax.axis_index("sp"), lax.axis_index("tp")
        return {
            "sp": s,
            "x": t,
            "c": lax.rem(s, self.c),
            "y": lax.rem(s // self.c, self.y),
            "z": s // (self.c * self.y),
        }

    def peer(self, place, dim, index):
        if dim == "sp":
            return {"sp": index, "tp": place["x"]}
        at = dict(place)
        at[dim] = index
        return {"sp": (at["z"] * self.y + at["y"]) * self.c + at["c"], "tp": at["x"]}

    def greet(self, place, dims):
        barrier = pltpu.get_barrier_semaphore()
        count = 0
        for dim in dims:
            n = self.size(dim)
            for k in range(1, n):
                peer = self.peer(place, dim, lax.rem(place[dim] + k, n))
                pl.semaphore_signal(barrier, inc=1, device_id=peer, device_id_type=MESH)
                count += 1
        pl.semaphore_wait(barrier, count)


def exchange_kernel(grid, dims, keep, *refs):
    m = len(dims)
    ins, outs = refs[:m], refs[m : 2 * m]
    send_sem, recv_sem, own_sem = refs[2 * m :]
    place = grid.place()
    copies = []
    grid.greet(place, sorted(set(dims)))
    base = 0
    for i, dim in enumerate(dims):
        n, me = grid.size(dim), place[dim]
        for k in range(1, n):
            to = lax.rem(me + k, n)
            slot = me if keep else k - 1
            copy = pltpu.make_async_remote_copy(
                src_ref=ins[i].at[to],
                dst_ref=outs[i].at[slot],
                send_sem=send_sem.at[base + k - 1],
                recv_sem=recv_sem.at[base + k - 1],
                device_id=grid.peer(place, dim, to),
                device_id_type=MESH,
            )
            copy.start()
            copies.append(copy)
        base += n - 1
    if keep:
        for i, dim in enumerate(dims):
            me = place[dim]
            own = pltpu.make_async_copy(ins[i].at[me], outs[i].at[me], own_sem.at[i])
            own.start()
            copies.append(own)
    for copy in copies:
        copy.wait()


def exchange(grid, items, keep):
    dims = tuple(d for _, d in items)
    total = sum(grid.size(d) - 1 for d in dims)
    shapes = tuple(
        jax.ShapeDtypeStruct(a.shape if keep else (a.shape[0] - 1,) + a.shape[1:], a.dtype)
        for a, _ in items
    )
    return pl.pallas_call(
        functools.partial(exchange_kernel, grid, dims, keep),
        out_shape=shapes,
        in_specs=[pl.BlockSpec(memory_space=pl.ANY)] * len(items),
        out_specs=[pl.BlockSpec(memory_space=pl.ANY)] * len(items),
        scratch_shapes=[
            pltpu.SemaphoreType.DMA((total,)),
            pltpu.SemaphoreType.DMA((total,)),
            pltpu.SemaphoreType.DMA((len(items),)),
        ],
        compiler_params=pltpu.CompilerParams(
            collective_id=next(grid.ids), has_side_effects=True
        ),
    )(*[a for a, _ in items])


def gather_kernel(grid, x_ref, out_ref, send_sem, recv_sem, own_sem):
    place = grid.place()
    z, y, c, x = (place[d] for d in "zycx")
    half = x_ref.shape[1] // 2
    first, second = pl.ds(0, half), pl.ds(half, half)
    everything = slice(None)
    grid.greet(place, ("z", "y", "c", "x"))
    own = pltpu.make_async_copy(x_ref, out_ref.at[z, y, c, x], own_sem)
    own.start()
    used = 0

    def push(dim, src, dst):
        nonlocal used
        n, copies = grid.size(dim), []
        for k in range(1, n):
            copy = pltpu.make_async_remote_copy(
                src_ref=src,
                dst_ref=dst,
                send_sem=send_sem.at[used],
                recv_sem=recv_sem.at[used],
                device_id=grid.peer(place, dim, lax.rem(place[dim] + k, n)),
                device_id_type=MESH,
            )
            copy.start()
            copies.append(copy)
            used += 1
        return copies

    stage = push("z", x_ref, out_ref.at[z, y, c, x])
    own.wait()
    for copy in stage:
        copy.wait()
    a = out_ref.at[:, y, c, x, :, first]
    b = out_ref.at[:, y, c, x, :, second]
    stage = push("y", a, a) + push("x", b, b)
    for copy in stage:
        copy.wait()
    a = out_ref.at[:, :, c, x, :, first]
    b = out_ref.at[:, y, c, :, :, second]
    stage = push("x", a, a) + push("y", b, b)
    for copy in stage:
        copy.wait()
    a = out_ref.at[:, :, c]
    for copy in push("c", a, a):
        copy.wait()


def gather(grid, array):
    total = sum(grid.size(d) - 1 for d in "zyyxxc")
    return pl.pallas_call(
        functools.partial(gather_kernel, grid),
        out_shape=jax.ShapeDtypeStruct(
            (grid.z, grid.y, grid.c, grid.x) + array.shape, array.dtype
        ),
        in_specs=[pl.BlockSpec(memory_space=pltpu.VMEM)],
        out_specs=pl.BlockSpec(memory_space=pl.ANY),
        scratch_shapes=[
            pltpu.SemaphoreType.DMA((total,)),
            pltpu.SemaphoreType.DMA((total,)),
            pltpu.SemaphoreType.DMA,
        ],
        compiler_params=pltpu.CompilerParams(
            collective_id=next(grid.ids), has_side_effects=True
        ),
    )(array)


def reduce_scatter(grid, first, second):
    place = grid.place()

    def stage(items):
        got = exchange(grid, items, False)
        sums = []
        for (array, dim), other in zip(items, got):
            own = lax.dynamic_index_in_dim(array, place[dim], 0, keepdims=False)
            sums.append(own.astype(F32) + jnp.sum(other.astype(F32), axis=0))
        return sums

    for dims in ("cc", "xy", "yx", "zz"):
        first, second = stage([(first.astype(BF16), dims[0]), (second.astype(BF16), dims[1])])
    return jnp.concatenate([first, second], axis=-1)


def dot(a, b, dims, precision=None):
    return lax.dot_general(
        a, b, (dims, ((), ())), precision=precision, preferred_element_type=F32
    )


def local_kernel(
    heads, zf_ref, zb_ref, v_ref, q_ref, floor_ref, extra_ref, out_ref, carry_ref, state_ref, decay_ref
):
    length = v_ref.shape[0]
    rows = lax.broadcasted_iota(jnp.int32, (length, length), 0)
    cols = lax.broadcasted_iota(jnp.int32, (length, length), 1)
    middle = length // 2
    for h in range(heads):
        at = slice(h * HEAD_WIDTH, (h + 1) * HEAD_WIDTH)
        values = v_ref[:, at]
        logits = q_ref[:, at].astype(F32)
        queries = logits * jax.nn.sigmoid(logits)
        scores = jnp.zeros((length, length), F32)
        for d, z_ref in enumerate((zf_ref, zb_ref)):
            mask = rows >= cols if d == 0 else rows <= cols
            z = z_ref[:, at].astype(F32)
            floor = floor_ref[d : d + 1, at]
            rest = 1.0 - floor
            logf = jnp.log(floor + rest * jax.nn.sigmoid(z)) + extra_ref[d, :, h : h + 1]
            key = rest * jax.nn.sigmoid(-z)
            running = dot(
                jnp.where(mask, 1.0, 0.0), logf, ((1,), (0,)), lax.Precision.HIGHEST
            )
            last = length - 1 if d == 0 else 0
            total = running[last : last + 1]
            centred = running - running[middle : middle + 1]
            part = dot(
                (queries * jnp.exp(centred)).astype(BF16),
                (key * jnp.exp(-centred)).astype(BF16),
                ((1,), (1,)),
            )
            scores += jnp.where(mask, part, 0.0)
            carry_ref[d, :, at] = (queries * jnp.exp(running)).astype(BF16)
            fresh = (key * jnp.exp(total - running)).astype(BF16)
            state_ref[d, h] = dot(values, fresh, ((0,), (0,))).astype(BF16)
            decay_ref[d, h] = jnp.broadcast_to(
                jnp.exp(total), (DECAY_ROWS, HEAD_WIDTH)
            ).astype(BF16)
        out_ref[:, at] = dot(scores.astype(BF16), values, ((1,), (0,)))


def prefix_kernel(rows, got_ref, out_ref):
    n = got_ref.shape[0]
    forward = lax.axis_index("sp") < n // 2

    def hop(k, carry):
        at = jnp.where(forward, k, n - 1 - k)
        out_ref[at] = carry.astype(BF16)
        block = got_ref[at].astype(F32)
        return block[rows : rows + 1] * carry + block[:rows]

    lax.fori_loop(0, n, hop, jnp.zeros((rows, HEAD_WIDTH), F32))


def finish_kernel(heads, out_ref, carry_ref, enter_ref, gate_ref, scale_ref, gated_ref):
    for h in range(heads):
        at = slice(h * HEAD_WIDTH, (h + 1) * HEAD_WIDTH)
        total = out_ref[:, at]
        for d in range(2):
            total += dot(carry_ref[d, :, at], enter_ref[d, h], ((1,), (1,)))
        mean = jnp.mean(total * total, axis=-1, keepdims=True)
        g = gate_ref[:, at].astype(F32)
        gated_ref[:, at] = (
            total * lax.rsqrt(mean + EPSILON) * scale_ref[...] * (g * jax.nn.sigmoid(g))
        ).astype(BF16)


def on_device(
    grid,
    residual,
    forget_forward,
    forget_backward,
    value_written,
    query_logits,
    output_gate_logits,
    forget_minimum,
    extra_log_rate,
    head_norm_scale,
    output_matrix,
    prenorm_scale,
    gate_up_matrix,
    value_up_matrix,
    gate_taps,
    value_taps,
    down_matrix,
):
    sp, tp = grid.sp, grid.x
    length, width = value_written.shape
    heads = width // HEAD_WIDTH
    depth, units = gate_up_matrix.shape
    unit = units // sp
    me = lax.axis_index("sp")

    out_full = lax.all_gather(output_matrix, "sp", axis=1, tiled=True)

    def cut(w):
        return w.reshape(depth, sp, unit).transpose(1, 0, 2)

    up = jnp.concatenate([cut(gate_up_matrix), cut(value_up_matrix)], axis=2)
    down = down_matrix.reshape(sp, unit, down_matrix.shape[1])
    up, down = exchange(grid, [(up, "sp"), (down, "sp")], True)
    up = up.reshape(sp * depth, 2 * unit)
    down = down.transpose(1, 0, 2).reshape(unit, -1)

    local, carry, state, decay = pl.pallas_call(
        functools.partial(local_kernel, heads),
        out_shape=(
            jax.ShapeDtypeStruct((length, width), F32),
            jax.ShapeDtypeStruct((2, length, width), BF16),
            jax.ShapeDtypeStruct((2, heads, HEAD_WIDTH, HEAD_WIDTH), BF16),
            jax.ShapeDtypeStruct((2, heads, DECAY_ROWS, HEAD_WIDTH), BF16),
        ),
    )(forget_forward, forget_backward, value_written, query_logits, forget_minimum, extra_log_rate)

    rows = 2 * heads * HEAD_WIDTH // sp
    decays = jnp.repeat(
        decay.reshape(2 * heads, DECAY_ROWS, HEAD_WIDTH), sp // (2 * heads), axis=0
    )
    message = jnp.concatenate([state.reshape(sp, rows, HEAD_WIDTH), decays], axis=1)
    (got,) = exchange(grid, [(message, "sp")], True)
    prefix = pl.pallas_call(
        functools.partial(prefix_kernel, rows),
        out_shape=jax.ShapeDtypeStruct((sp, rows, HEAD_WIDTH), BF16),
    )(got)
    (entering,) = exchange(grid, [(prefix, "sp")], True)
    gated = pl.pallas_call(
        functools.partial(finish_kernel, heads),
        out_shape=jax.ShapeDtypeStruct((length, width), BF16),
    )(
        local,
        carry,
        entering.reshape(2, heads, HEAD_WIDTH, HEAD_WIDTH),
        output_gate_logits,
        head_norm_scale[None],
    )
    (swapped,) = exchange(grid, [(gated.reshape(tp, length // tp, width), "x")], True)
    token_rows = swapped.transpose(1, 0, 2).reshape(length // tp, tp * width)
    mixed = jnp.dot(token_rows, out_full, preferred_element_type=F32)
    own_after = residual.astype(F32) + mixed
    mean = jnp.mean(own_after * own_after, axis=-1, keepdims=True)
    normed = (own_after * lax.rsqrt(mean + EPSILON) * prenorm_scale).astype(BF16)
    everyone = gather(grid, normed)
    tokens = everyone.reshape(-1, normed.shape[1])
    upward = jnp.dot(tokens, up, preferred_element_type=F32).astype(BF16)
    padded = jnp.pad(upward, ((1, 1), (0, 0)))
    taps = jnp.concatenate(
        [
            lax.dynamic_slice_in_dim(gate_taps, me * unit, unit, 1),
            lax.dynamic_slice_in_dim(value_taps, me * unit, unit, 1),
        ],
        axis=1,
    )
    count = tokens.shape[0]
    conv = padded[:count] * taps[0] + padded[1 : count + 1] * taps[1] + padded[2:] * taps[2]
    hidden = (jax.nn.silu(conv[:, :unit]) * conv[:, unit:]).astype(BF16)
    parts = hidden.reshape(everyone.shape[:-1] + (unit,))
    half = down.shape[1] // 2

    def project(order, weights):
        moved = parts.transpose(*order, 4, 5)
        product = jnp.dot(moved.reshape(-1, unit), weights, preferred_element_type=F32)
        return product.astype(BF16).reshape(moved.shape[:-1] + (weights.shape[1],))

    down_sum = reduce_scatter(
        grid, project((2, 3, 1, 0), down[:, :half]), project((2, 1, 3, 0), down[:, half:])
    )
    return (own_after + down_sum).astype(BF16)


def solution(mesh):
    return jax.shard_map(
        functools.partial(on_device, Grid(mesh)),
        mesh=mesh,
        in_specs=(
            P(("sp", "tp"), None),
            P("sp", "tp"),
            P("sp", "tp"),
            P("sp", "tp"),
            P("sp", "tp"),
            P("sp", "tp"),
            P(None, "tp"),
            P(None, "sp", "tp"),
            P(),
            P(None, "sp"),
            P(),
            P("sp", "tp"),
            P("sp", "tp"),
            P(None, "tp"),
            P(None, "tp"),
            P("tp", "sp"),
        ),
        out_specs=P(("sp", "tp"), None),
        check_vma=False,
    )
```

```python
import functools
import math

import jax
import jax.numpy as jnp
from jax import lax
from jax.experimental import pallas as pl
from jax.experimental.pallas import tpu as pltpu
from jax.sharding import PartitionSpec as P

HEAD_WIDTH = 128
EPSILON = 1e-06
MESH = pl.DeviceIdType.MESH
F32 = jnp.float32
BF16 = jnp.bfloat16
DECAY_ROWS = 16
CHUNKS = 4


class Grid:
    def __init__(self, mesh):
        sp, tp = mesh.shape["sp"], mesh.shape["tp"]
        self.sp, self.x = sp, tp
        self.c = math.gcd(sp, 2)
        self.y = math.gcd(sp // self.c, 2)
        self.z = sp // (self.c * self.y)
        self.ids = iter(range(100))

    def size(self, dim):
        return getattr(self, dim)

    def place(self):
        s, t = lax.axis_index("sp"), lax.axis_index("tp")
        return {
            "sp": s,
            "x": t,
            "c": lax.rem(s, self.c),
            "y": lax.rem(s // self.c, self.y),
            "z": s // (self.c * self.y),
        }

    def peer(self, place, dim, index):
        if dim == "sp":
            return {"sp": index, "tp": place["x"]}
        at = dict(place)
        at[dim] = index
        return {"sp": (at["z"] * self.y + at["y"]) * self.c + at["c"], "tp": at["x"]}

    def greet(self, place, dims):
        barrier = pltpu.get_barrier_semaphore()
        count = 0
        for dim in dims:
            n = self.size(dim)
            for k in range(1, n):
                peer = self.peer(place, dim, lax.rem(place[dim] + k, n))
                pl.semaphore_signal(barrier, inc=1, device_id=peer, device_id_type=MESH)
                count += 1
        pl.semaphore_wait(barrier, count)


def exchange_kernel(grid, dims, keep, *refs):
    m = len(dims)
    ins, outs = refs[:m], refs[m : 2 * m]
    send_sem, recv_sem, own_sem = refs[2 * m :]
    place = grid.place()
    copies = []
    grid.greet(place, sorted(set(dims)))
    base = 0
    for i, dim in enumerate(dims):
        n, me = grid.size(dim), place[dim]
        for k in range(1, n):
            to = lax.rem(me + k, n)
            slot = me if keep else k - 1
            copy = pltpu.make_async_remote_copy(
                src_ref=ins[i].at[to],
                dst_ref=outs[i].at[slot],
                send_sem=send_sem.at[base + k - 1],
                recv_sem=recv_sem.at[base + k - 1],
                device_id=grid.peer(place, dim, to),
                device_id_type=MESH,
            )
            copy.start()
            copies.append(copy)
        base += n - 1
    if keep:
        for i, dim in enumerate(dims):
            me = place[dim]
            own = pltpu.make_async_copy(ins[i].at[me], outs[i].at[me], own_sem.at[i])
            own.start()
            copies.append(own)
    for copy in copies:
        copy.wait()


def exchange(grid, items, keep):
    dims = tuple(d for _, d in items)
    total = sum(grid.size(d) - 1 for d in dims)
    shapes = tuple(
        jax.ShapeDtypeStruct(a.shape if keep else (a.shape[0] - 1,) + a.shape[1:], a.dtype)
        for a, _ in items
    )
    return pl.pallas_call(
        functools.partial(exchange_kernel, grid, dims, keep),
        out_shape=shapes,
        in_specs=[pl.BlockSpec(memory_space=pl.ANY)] * len(items),
        out_specs=[pl.BlockSpec(memory_space=pl.ANY)] * len(items),
        scratch_shapes=[
            pltpu.SemaphoreType.DMA((total,)),
            pltpu.SemaphoreType.DMA((total,)),
            pltpu.SemaphoreType.DMA((len(items),)),
        ],
        compiler_params=pltpu.CompilerParams(
            collective_id=next(grid.ids), has_side_effects=True
        ),
    )(*[a for a, _ in items])


def gather_kernel(grid, x_ref, out_ref, send_sem, recv_sem, own_sem):
    place = grid.place()
    z, y, c, x = (place[d] for d in "zycx")
    part = x_ref.shape[1] // (2 * CHUNKS)
    grid.greet(place, ("z", "y", "c", "x"))
    own = pltpu.make_async_copy(x_ref, out_ref.at[z, y, c, x], own_sem)
    own.start()
    used = 0

    def push(dim, src, dst):
        nonlocal used
        n, copies = grid.size(dim), []
        for k in range(1, n):
            copy = pltpu.make_async_remote_copy(
                src_ref=src,
                dst_ref=dst,
                send_sem=send_sem.at[used],
                recv_sem=recv_sem.at[used],
                device_id=grid.peer(place, dim, lax.rem(place[dim] + k, n)),
                device_id_type=MESH,
            )
            copy.start()
            copies.append(copy)
            used += 1
        return copies

    def start(level, t):
        both = pl.ds(2 * t * part, 2 * part)
        first, second = pl.ds(2 * t * part, part), pl.ds((2 * t + 1) * part, part)
        if level == 0:
            return push("z", x_ref.at[:, both], out_ref.at[z, y, c, x, :, both])
        if level == 1:
            a = out_ref.at[:, y, c, x, :, first]
            b = out_ref.at[:, y, c, x, :, second]
            return push("y", a, a) + push("x", b, b)
        if level == 2:
            a = out_ref.at[:, :, c, x, :, first]
            b = out_ref.at[:, y, c, :, :, second]
            return push("x", a, a) + push("y", b, b)
        a = out_ref.at[:, :, c, :, :, both]
        return push("c", a, a)

    flying = {(0, t): start(0, t) for t in range(CHUNKS)}
    own.wait()
    for step in range(CHUNKS + 3):
        for level in range(4):
            t = step - level
            if 0 <= t < CHUNKS:
                for copy in flying[level, t]:
                    copy.wait()
                if level < 3:
                    flying[level + 1, t] = start(level + 1, t)


def gather(grid, array):
    total = CHUNKS * sum(grid.size(d) - 1 for d in "zyyxxc")
    return pl.pallas_call(
        functools.partial(gather_kernel, grid),
        out_shape=jax.ShapeDtypeStruct(
            (grid.z, grid.y, grid.c, grid.x) + array.shape, array.dtype
        ),
        in_specs=[pl.BlockSpec(memory_space=pltpu.VMEM)],
        out_specs=pl.BlockSpec(memory_space=pl.ANY),
        scratch_shapes=[
            pltpu.SemaphoreType.DMA((total,)),
            pltpu.SemaphoreType.DMA((total,)),
            pltpu.SemaphoreType.DMA,
        ],
        compiler_params=pltpu.CompilerParams(
            collective_id=next(grid.ids), has_side_effects=True
        ),
    )(array)


ORDERS = ("cxyz", "cyxz")


def reduce_kernel(grid, a_ref, b_ref, out_ref, *scratch):
    held, got, (send_sem, recv_sem, own_sem) = scratch[:2], scratch[2:10], scratch[10:]
    terms = (a_ref, b_ref)
    place = grid.place()
    rows, part = held[0].shape[-2:]
    grid.greet(place, ("z", "y", "c", "x"))
    used = 0

    def start(level, t):
        nonlocal used
        copies = []
        for color in range(2):
            dim = ORDERS[color][level]
            n, me = grid.size(dim), place[dim]
            for k in range(1, n):
                to = lax.rem(me + k, n)
                if level == 0:
                    src = terms[color].at[to, :, :, :, :, pl.ds(t * part, part)]
                else:
                    before = tuple(place[d] for d in ORDERS[color][1:level])
                    src = held[color].at[(t,) + before + (to,)]
                copy = pltpu.make_async_remote_copy(
                    src_ref=src,
                    dst_ref=got[2 * level + color].at[t, k - 1],
                    send_sem=send_sem.at[used],
                    recv_sem=recv_sem.at[used],
                    device_id=grid.peer(place, dim, to),
                    device_id_type=MESH,
                )
                copy.start()
                copies.append(copy)
                used += 1
        return copies

    def add(level, t):
        for color in range(2):
            order = ORDERS[color]
            here = tuple(place[d] for d in order[1 : level + 1])
            left = [grid.size(d) for d in order[level + 1 :]]
            peers = grid.size(order[level]) - 1
            where = got[2 * level + color]

            def block(i, _, color=color, here=here, left=left, peers=peers, where=where):
                index, rest = [], i
                for n in reversed(left):
                    index.insert(0, lax.rem(rest, n))
                    rest = rest // n
                index = tuple(index)
                total = held[color][(t,) + here + index].astype(F32)
                for k in range(peers):
                    total += where[(t, k) + index].astype(F32)
                if level < 3:
                    held[color][(t,) + here + index] = total.astype(BF16)
                else:
                    first = (color * CHUNKS + t) * part
                    out_ref[:, first : first + part] = total
                return 0

            if left:
                lax.fori_loop(0, math.prod(left), block, 0)
            else:
                block(0, 0)

    flying = {(0, t): start(0, t) for t in range(CHUNKS)}
    for t in range(CHUNKS):
        for color in range(2):
            own = pltpu.make_async_copy(
                terms[color].at[place["c"], :, :, :, :, pl.ds(t * part, part)],
                held[color].at[t],
                own_sem.at[t, color],
            )
            own.start()
            flying[0, t].append(own)
    for step in range(CHUNKS + 3):
        for level in range(4):
            t = step - level
            if 0 <= t < CHUNKS:
                for copy in flying[level, t]:
                    copy.wait()
                add(level, t)
                if level < 3:
                    flying[level + 1, t] = start(level + 1, t)


def reduce_scatter(grid, first, second):
    rows, cols = first.shape[-2:]
    tile = (rows, cols // CHUNKS)

    def sizes(order):
        return tuple(grid.size(d) for d in order)

    scratch = [pltpu.VMEM((CHUNKS,) + sizes(o[1:]) + tile, BF16) for o in ORDERS]
    for level in range(4):
        for o in ORDERS:
            peers = grid.size(o[level]) - 1
            scratch.append(
                pltpu.VMEM((CHUNKS, max(peers, 1)) + sizes(o[level + 1 :]) + tile, BF16)
            )
    total = 2 * CHUNKS * sum(grid.size(d) - 1 for d in "cxyz")
    return pl.pallas_call(
        functools.partial(reduce_kernel, grid),
        out_shape=jax.ShapeDtypeStruct((rows, 2 * cols), F32),
        in_specs=[pl.BlockSpec(memory_space=pl.ANY)] * 2,
        out_specs=pl.BlockSpec(memory_space=pltpu.VMEM),
        scratch_shapes=scratch
        + [
            pltpu.SemaphoreType.DMA((total,)),
            pltpu.SemaphoreType.DMA((total,)),
            pltpu.SemaphoreType.DMA((CHUNKS, 2)),
        ],
        compiler_params=pltpu.CompilerParams(
            collective_id=next(grid.ids), has_side_effects=True, vmem_limit_bytes=64000000
        ),
    )(first, second)


def dot(a, b, dims, precision=None):
    return lax.dot_general(
        a, b, (dims, ((), ())), precision=precision, preferred_element_type=F32
    )


def local_kernel(
    heads, zf_ref, zb_ref, v_ref, q_ref, floor_ref, extra_ref, out_ref, carry_ref, state_ref, decay_ref
):
    length = v_ref.shape[0]
    rows = lax.broadcasted_iota(jnp.int32, (length, length), 0)
    cols = lax.broadcasted_iota(jnp.int32, (length, length), 1)
    middle = length // 2
    for h in range(heads):
        at = slice(h * HEAD_WIDTH, (h + 1) * HEAD_WIDTH)
        values = v_ref[:, at]
        logits = q_ref[:, at].astype(F32)
        queries = logits * jax.nn.sigmoid(logits)
        scores = jnp.zeros((length, length), F32)
        for d, z_ref in enumerate((zf_ref, zb_ref)):
            mask = rows >= cols if d == 0 else rows <= cols
            z = z_ref[:, at].astype(F32)
            floor = floor_ref[d : d + 1, at]
            rest = 1.0 - floor
            logf = jnp.log(floor + rest * jax.nn.sigmoid(z)) + extra_ref[d, :, h : h + 1]
            key = rest * jax.nn.sigmoid(-z)
            running = dot(
                jnp.where(mask, 1.0, 0.0), logf, ((1,), (0,)), lax.Precision.HIGHEST
            )
            last = length - 1 if d == 0 else 0
            total = running[last : last + 1]
            centred = running - running[middle : middle + 1]
            part = dot(
                (queries * jnp.exp(centred)).astype(BF16),
                (key * jnp.exp(-centred)).astype(BF16),
                ((1,), (1,)),
            )
            scores += jnp.where(mask, part, 0.0)
            carry_ref[d, :, at] = (queries * jnp.exp(running)).astype(BF16)
            fresh = (key * jnp.exp(total - running)).astype(BF16)
            state_ref[d, h] = dot(values, fresh, ((0,), (0,))).astype(BF16)
            decay_ref[d, h] = jnp.broadcast_to(
                jnp.exp(total), (DECAY_ROWS, HEAD_WIDTH)
            ).astype(BF16)
        out_ref[:, at] = dot(scores.astype(BF16), values, ((1,), (0,)))


def prefix_kernel(rows, got_ref, out_ref):
    n = got_ref.shape[0]
    forward = lax.axis_index("sp") < n // 2

    def hop(k, carry):
        at = jnp.where(forward, k, n - 1 - k)
        out_ref[at] = carry.astype(BF16)
        block = got_ref[at].astype(F32)
        return block[rows : rows + 1] * carry + block[:rows]

    lax.fori_loop(0, n, hop, jnp.zeros((rows, HEAD_WIDTH), F32))


def finish_kernel(heads, out_ref, carry_ref, enter_ref, gate_ref, scale_ref, gated_ref):
    for h in range(heads):
        at = slice(h * HEAD_WIDTH, (h + 1) * HEAD_WIDTH)
        total = out_ref[:, at]
        for d in range(2):
            total += dot(carry_ref[d, :, at], enter_ref[d, h], ((1,), (1,)))
        mean = jnp.mean(total * total, axis=-1, keepdims=True)
        g = gate_ref[:, at].astype(F32)
        gated_ref[:, at] = (
            total * lax.rsqrt(mean + EPSILON) * scale_ref[...] * (g * jax.nn.sigmoid(g))
        ).astype(BF16)


def on_device(
    grid,
    residual,
    forget_forward,
    forget_backward,
    value_written,
    query_logits,
    output_gate_logits,
    forget_minimum,
    extra_log_rate,
    head_norm_scale,
    output_matrix,
    prenorm_scale,
    gate_up_matrix,
    value_up_matrix,
    gate_taps,
    value_taps,
    down_matrix,
):
    sp, tp = grid.sp, grid.x
    length, width = value_written.shape
    heads = width // HEAD_WIDTH
    depth, units = gate_up_matrix.shape
    unit = units // sp
    me = lax.axis_index("sp")

    out_full = lax.all_gather(output_matrix, "sp", axis=1, tiled=True)

    def cut(w):
        return w.reshape(depth, sp, unit).transpose(1, 0, 2)

    up = jnp.concatenate([cut(gate_up_matrix), cut(value_up_matrix)], axis=2)
    down = down_matrix.reshape(sp, unit, down_matrix.shape[1])
    up, down = exchange(grid, [(up, "sp"), (down, "sp")], True)
    up = up.reshape(sp * depth, 2 * unit)
    down = down.transpose(1, 0, 2).reshape(unit, -1)

    local, carry, state, decay = pl.pallas_call(
        functools.partial(local_kernel, heads),
        out_shape=(
            jax.ShapeDtypeStruct((length, width), F32),
            jax.ShapeDtypeStruct((2, length, width), BF16),
            jax.ShapeDtypeStruct((2, heads, HEAD_WIDTH, HEAD_WIDTH), BF16),
            jax.ShapeDtypeStruct((2, heads, DECAY_ROWS, HEAD_WIDTH), BF16),
        ),
    )(forget_forward, forget_backward, value_written, query_logits, forget_minimum, extra_log_rate)

    rows = 2 * heads * HEAD_WIDTH // sp
    decays = jnp.repeat(
        decay.reshape(2 * heads, DECAY_ROWS, HEAD_WIDTH), sp // (2 * heads), axis=0
    )
    message = jnp.concatenate([state.reshape(sp, rows, HEAD_WIDTH), decays], axis=1)
    (got,) = exchange(grid, [(message, "sp")], True)
    prefix = pl.pallas_call(
        functools.partial(prefix_kernel, rows),
        out_shape=jax.ShapeDtypeStruct((sp, rows, HEAD_WIDTH), BF16),
    )(got)
    (entering,) = exchange(grid, [(prefix, "sp")], True)
    gated = pl.pallas_call(
        functools.partial(finish_kernel, heads),
        out_shape=jax.ShapeDtypeStruct((length, width), BF16),
    )(
        local,
        carry,
        entering.reshape(2, heads, HEAD_WIDTH, HEAD_WIDTH),
        output_gate_logits,
        head_norm_scale[None],
    )
    (swapped,) = exchange(grid, [(gated.reshape(tp, length // tp, width), "x")], True)
    token_rows = swapped.transpose(1, 0, 2).reshape(length // tp, tp * width)
    mixed = jnp.dot(token_rows, out_full, preferred_element_type=F32)
    own_after = residual.astype(F32) + mixed
    mean = jnp.mean(own_after * own_after, axis=-1, keepdims=True)
    normed = (own_after * lax.rsqrt(mean + EPSILON) * prenorm_scale).astype(BF16)
    everyone = gather(grid, normed)
    tokens = everyone.reshape(-1, normed.shape[1])
    upward = jnp.dot(tokens, up, preferred_element_type=F32).astype(BF16)
    padded = jnp.pad(upward, ((1, 1), (0, 0)))
    taps = jnp.concatenate(
        [
            lax.dynamic_slice_in_dim(gate_taps, me * unit, unit, 1),
            lax.dynamic_slice_in_dim(value_taps, me * unit, unit, 1),
        ],
        axis=1,
    )
    count = tokens.shape[0]
    conv = padded[:count] * taps[0] + padded[1 : count + 1] * taps[1] + padded[2:] * taps[2]
    hidden = (jax.nn.silu(conv[:, :unit]) * conv[:, unit:]).astype(BF16)
    parts = hidden.reshape(everyone.shape[:-1] + (unit,))
    half = down.shape[1] // 2

    def project(order, weights):
        moved = parts.transpose(*order, 4, 5)
        product = jnp.dot(moved.reshape(-1, unit), weights, preferred_element_type=F32)
        return product.astype(BF16).reshape(moved.shape[:-1] + (weights.shape[1],))

    down_sum = reduce_scatter(
        grid, project((2, 3, 1, 0), down[:, :half]), project((2, 1, 3, 0), down[:, half:])
    )
    return (own_after + down_sum).astype(BF16)


def solution(mesh):
    return jax.shard_map(
        functools.partial(on_device, Grid(mesh)),
        mesh=mesh,
        in_specs=(
            P(("sp", "tp"), None),
            P("sp", "tp"),
            P("sp", "tp"),
            P("sp", "tp"),
            P("sp", "tp"),
            P("sp", "tp"),
            P(None, "tp"),
            P(None, "sp", "tp"),
            P(),
            P(None, "sp"),
            P(),
            P("sp", "tp"),
            P("sp", "tp"),
            P(None, "tp"),
            P(None, "tp"),
            P("tp", "sp"),
        ),
        out_specs=P(("sp", "tp"), None),
        check_vma=False,
    )
```
